32 devices in a mesh: ep: 8 (over z, y), tp: 4 (over x, core).
Axes of the slice: x: 2, y: 2, z: 4, core: 2. Of those that a mesh axis runs over, the one named last changes fastest.
Arguments:
- query_rows: bfloat16 [1024, 1024], P('ep', 'tp'), may hold values from -10 to 10
- key_rows: bfloat16 [1024, 1024], P('ep', 'tp'), may hold values from -10 to 10
- value_rows: bfloat16 [1024, 1024], P('ep', 'tp'), may hold values from -6 to 6
- key_bias: bfloat16 [1024, 16], P('ep', 'tp'), may hold values from -24 to 4
- mixer_weight: bfloat16 [1024, 2048], P('tp'), may hold values from -0.1875 to 0.1875
- mixer_gain: float32 [2048], replicated, may hold values from 0.1 to 1.9
- routed_input: bfloat16 [3072, 2048], P(('ep', 'tp')), may hold values from -6 to 6
- entry_gain: float32 [2048], replicated, may hold values from 0.1 to 1.9
- expert_index: int32 [3072, 2], P(('ep', 'tp')), may hold values from 0 to 15, all different within a row; in each aligned block of 96 rows (0 to 95, 96 to 191, ...) at most 18 rows name the same one
- route_weights: float32 [3072, 2], P(('ep', 'tp')), may hold values from 0.1 to 1
- expert_gate: bfloat16 [16, 2048, 1024], P('ep', None, 'tp'), may hold values from -0.125 to 0.125
- expert_up: bfloat16 [16, 2048, 1024], P('ep', None, 'tp'), may hold values from -0.125 to 0.125
- expert_down: bfloat16 [16, 1024, 2048], P('ep', 'tp'), may hold values from -0.1875 to 0.1875
- shared_gate: bfloat16 [2048, 1024], P(None, 'tp'), may hold values from -0.125 to 0.125
- shared_up: bfloat16 [2048, 1024], P(None, 'tp'), may hold values from -0.125 to 0.125
- shared_down: bfloat16 [1024, 2048], P('tp'), may hold values from -0.1875 to 0.1875
- exit_gain: float32 [2048], replicated, may hold values from 0.1 to 1.9
Outputs:
- mixer_out: bfloat16 [1024, 2048], P(('ep', 'tp'))
- expert_out: bfloat16 [3072, 2048], P(('ep', 'tp'))
The draws below stay inside these ranges and needn't reach their ends.
Inputs may be any that keep to these rules, and one draw needn't show every extreme that they name: `expert_index`: in each aligned block of 96 rows (the rows of one device) no expert is named by more than 18 rows, a bound that some block reaches; each row names 2 different experts.
All inputs are finite; a program needn't handle non-finite values.
Results may differ from the reference program's by a relative error of at most 0.012.
Values may be sent and summed in bfloat16 or wider, within the bound.
A program may use at most 128 MiB of HBM per device.

```python
import math
import jax
import jax.numpy as jnp
import numpy as np
from jax import lax

D = 2048
HEADS = 16
HEAD_DIM = 64
FF = 1024
FF_SH = 1024
TOPK = 2
TOK_A = 128
ROWS_B = 96
TOKENS_A = 1024
TOKENS_B = 3072
EXPERTS = 16
CAP = 18
N_EP = 8
N_TP = 4


def draw_key_bias(key, part):
    random_subkeys = jax.random.split(key, 7)
    sequence_length = TOKENS_A
    head_count = HEADS
    head_draw = jax.random.uniform(random_subkeys[0], (head_count,))
    quick_heads = (head_draw < 0.5) | (head_draw <= jnp.min(head_draw))
    keep_share = jax.random.uniform(random_subkeys[1], (head_count,), minval=0.4, maxval=1.2)
    fast_reach = jax.random.uniform(random_subkeys[2], (head_count,), minval=30.0, maxval=50.0)
    noise_shift = 3.3
    slow_level = jnp.log(keep_share / sequence_length) - noise_shift
    fast_level = -jnp.log(fast_reach) - noise_shift
    base_level = jnp.where(quick_heads, fast_level, slow_level)
    shard_count = sequence_length // TOK_A
    shard_shift = jax.random.uniform(random_subkeys[3], (shard_count, head_count), minval=-0.7, maxval=0.7)
    shard_shift = jnp.repeat(shard_shift, TOK_A, axis=0)
    roughness = 0.3 * jax.random.normal(random_subkeys[4], (sequence_length, head_count))
    logarithm_bias = base_level[None, :] + shard_shift + roughness
    spike_positions = jax.random.randint(random_subkeys[5], (3,), 0, sequence_length)
    spike_rows = jnp.any(jnp.arange(sequence_length)[:, None] == spike_positions[None, :], axis=1)
    remaining_fraction = jax.random.uniform(random_subkeys[6], (sequence_length, head_count), minval=0.2, maxval=0.5)
    spike_level = jnp.log(remaining_fraction / (1.0 - remaining_fraction))
    logarithm_bias = jnp.where(spike_rows[:, None] & (~quick_heads)[None, :], spike_level, logarithm_bias)
    return logarithm_bias.astype(jnp.float32).astype(jnp.bfloat16)


def block_levels(key, dims, cuts, low, largest):
    level, own = 1.0, jax.random.fold_in(key, 6)
    for axis_at, blocks in cuts:
        heights = jnp.exp(jax.random.uniform(jax.random.fold_in(own, axis_at), (blocks,), jnp.float32, low / len(cuts), largest / len(cuts)))
        level = level * jnp.repeat(heights, dims[axis_at] // blocks).reshape([-1 if axis == axis_at else 1 for axis in range(len(dims))])
    return level


def deal_out(own_key, own, number, rows, number_of, top, reach, skew):
    ranking = jax.random.permutation(own_key, number_of)
    heavy_load, common = shares(number_of, rows * top, reach, skew, True), shares(number_of, rows * top, reach, skew, False)
    places = jnp.arange(number_of)

    def named(tallies, offset_by):
        used = int((tallies > 0).sum())
        fixed = max(1, used // 4)
        moved = fixed + (places - fixed + offset_by * (used - fixed)) % max(1, number_of - fixed)
        return jnp.zeros((number_of,), jnp.int32).at[ranking[jnp.where(places < fixed, places, moved)]].set(jnp.asarray(tallies, jnp.int32))

    tallies = jnp.where(number % 4 == 0, named(heavy_load, number // 4), named(common, number - number // 4 - 1))
    mixed = jax.random.permutation(jax.random.fold_in(own, 3), number_of)
    source_of, receiver = mixed[0:number_of // 2 * 2:2], mixed[1:number_of // 2 * 2:2]
    margin = jnp.minimum(tallies[source_of] - 1, reach - tallies[receiver]) // 2
    margin = jnp.where((source_of == ranking[0]) | (receiver == ranking[0]) | (tallies[receiver] == 0), 0, jnp.maximum(margin, 0))
    moved = jax.random.randint(jax.random.fold_in(own, 4), (number_of // 2,), 0, 1 << 20) % (margin + 1)
    tallies = tallies.at[source_of].add(-moved).at[receiver].add(moved)
    labels = jnp.searchsorted(jnp.cumsum(tallies), jnp.arange(rows * top), side="right").astype(jnp.int32)
    listing = labels.reshape(top, rows).T
    listing = listing[jax.random.permutation(jax.random.fold_in(own, 1), rows)]
    offset_by = jax.random.randint(jax.random.fold_in(own, 2), (rows, 1), 0, top)
    return jnp.take_along_axis(listing, (jnp.arange(top)[None, :] + offset_by) % top, axis=1)


def shares(count, total, bound, slope, full):
    loads = [(1 << 20) // math.isqrt(grade ** slope) + 1 for grade in range(1, count + 1)]
    largest = bound if full else min(bound, max(-(-total // count), total * loads[0] // sum(loads)))
    least = 1 if total - largest >= count - 1 else 0
    holding, surplus = [largest] + [least] * (count - 1), total - largest - least * (count - 1)
    while surplus > 0:
        movable = [i for i in range(1, count) if holding[i] < largest] or [i for i in range(1, count) if holding[i] < bound]
        whole, left = sum([loads[i] for i in movable]), surplus
        for i in movable:
            addition = min(bound - holding[i], max(1, left * loads[i] // whole), surplus)
            holding[i] = holding[i] + addition
            surplus = surplus - addition
    return np.array(holding)


def gaussian(rng, shape, deviation, bound, cuts=(), kind=jnp.bfloat16):
    array = jax.random.normal(rng, shape, jnp.float32) * deviation
    if len(cuts) > 0:
        array = block_levels(rng, shape, cuts, -0.22, 0.18) * array
    return jnp.clip(array, min=-bound, max=bound).astype(kind)


def setup_inputs(seed: int = 0) -> dict:
    seeds = jax.random.split(jax.random.key(seed), 18)
    query_rows = gaussian(seeds[0], (TOKENS_A, HEADS * HEAD_DIM), 1.6, 10.0, ((0, 8), (1, 4)))
    key_rows = gaussian(seeds[1], (TOKENS_A, HEADS * HEAD_DIM), 1.6, 10.0, ((0, 8), (1, 4)))
    value_rows = gaussian(seeds[2], (TOKENS_A, HEADS * HEAD_DIM), 1.0, 6.0, ((0, 8), (1, 4)))
    key_bias = draw_key_bias(jax.random.fold_in(seeds[17], 71), 0)
    mixer_weight = gaussian(seeds[4], (HEADS * HEAD_DIM, D), (HEADS * HEAD_DIM) ** -0.5, 0.1875, ((0, 4),))
    mixer_gain = jnp.clip(1.0 + 0.18 * jax.random.normal(seeds[5], (D,), jnp.float32), 0.1, 1.9)
    routed_input = gaussian(seeds[6], (TOKENS_B, D), 1.0, 6.0, ((0, 32),))
    entry_gain = jnp.clip(1.0 + 0.18 * jax.random.normal(seeds[7], (D,), jnp.float32), 0.1, 1.9)
    expert_index_keys = jax.random.split(jax.random.fold_in(seeds[8], 1), TOKENS_B // ROWS_B)
    expert_index_turns = jax.random.permutation(jax.random.fold_in(seeds[8], 3), TOKENS_B // ROWS_B)
    expert_index = jax.vmap(lambda own, number: deal_out(jax.random.fold_in(seeds[8], 2), own, number, ROWS_B, EXPERTS, TOPK, CAP, 2))(expert_index_keys, expert_index_turns).reshape((TOKENS_B, TOPK))
    route_weights = jnp.clip(jnp.exp(math.log(1.0) - 2.3025851 * jax.random.uniform(seeds[9], (TOKENS_B, TOPK), jnp.float32) ** block_levels(seeds[9], (TOKENS_B, TOPK), ((0, 32),), -0.2, 0.2)), 0.1, 1.0)
    expert_gate = gaussian(seeds[10], (EXPERTS, D, FF), D ** -0.5, 0.125, ((0, 8), (2, 4)))
    expert_up = gaussian(seeds[11], (EXPERTS, D, FF), D ** -0.5, 0.125, ((0, 8), (2, 4)))
    expert_down = gaussian(seeds[12], (EXPERTS, FF, D), FF ** -0.5, 0.1875, ((0, 8), (1, 4)))
    shared_gate = gaussian(seeds[13], (D, FF_SH), D ** -0.5, 0.125, ((1, 4),))
    shared_up = gaussian(seeds[14], (D, FF_SH), D ** -0.5, 0.125, ((1, 4),))
    shared_down = gaussian(seeds[15], (FF_SH, D), FF_SH ** -0.5, 0.1875, ((0, 4),))
    exit_gain = jnp.clip(1.0 + 0.18 * jax.random.normal(seeds[16], (D,), jnp.float32), 0.1, 1.9)
    return dict(query_rows=query_rows, key_rows=key_rows, value_rows=value_rows, key_bias=key_bias, mixer_weight=mixer_weight, mixer_gain=mixer_gain, routed_input=routed_input, entry_gain=entry_gain, expert_index=expert_index, route_weights=route_weights, expert_gate=expert_gate, expert_up=expert_up, expert_down=expert_down, shared_gate=shared_gate, shared_up=shared_up, shared_down=shared_down, exit_gain=exit_gain)


EPS = 1e-06

def root_norm(values, gain_row):
    return values * lax.rsqrt(lax.optimization_barrier(jnp.mean(values * values, axis=-1, keepdims=True)) + EPS) * gain_row

def key_shards():
    shards = 1
    while shards * TOK_A < 512 and N_EP % (2 * shards) == 0:
        shards = shards * 2
    return shards

def stick_breaking(query_rows, key_rows, value_rows, key_bias):
    total_rows = query_rows.shape[0]
    block_rows = key_shards() * TOK_A
    query_split = query_rows.reshape(N_EP, TOK_A, HEADS, HEAD_DIM).astype(jnp.float32)
    keys_split = key_rows.reshape(total_rows, HEADS, HEAD_DIM).astype(jnp.float32)
    values_split = value_rows.reshape(total_rows, HEADS, HEAD_DIM).astype(jnp.float32)
    bias_split = jnp.transpose(key_bias.astype(jnp.float32))
    score_scale = HEAD_DIM ** (-0.5)

    def one_shard(shard_pair):
        shard_query, shard_index = shard_pair
        query_pos = shard_index * TOK_A + jnp.arange(TOK_A, dtype=jnp.int32)
        own_block = shard_index * TOK_A // block_rows

        def backward_turn(turn_index, carried_pair):
            output, carried = carried_pair
            block_start = ((own_block - turn_index) * block_rows).astype(jnp.int32)
            block_keys = lax.dynamic_slice_in_dim(keys_split, block_start, block_rows, 0)
            block_values = lax.dynamic_slice_in_dim(values_split, block_start, block_rows, 0)
            block_bias = lax.dynamic_slice_in_dim(bias_split, block_start, block_rows, 1)
            scores = jnp.einsum('qhd,khd->hqk', shard_query, block_keys) * score_scale + block_bias[:, None, :]
            key_pos = block_start + jnp.arange(block_rows, dtype=jnp.int32)
            causal = (key_pos[None, :] < query_pos[:, None])[None]
            fail_logs = jnp.where(causal, -jax.nn.softplus(scores), 0.0)
            later_sum = lax.cumsum(fail_logs, axis=2, reverse=True) - fail_logs + carried[:, :, None]
            weights = jnp.where(causal, jnp.exp(jax.nn.log_sigmoid(scores) + later_sum), 0.0)
            weights = lax.optimization_barrier(weights.astype(jnp.bfloat16)).astype(jnp.float32)
            output = output + jnp.einsum('hqk,khd->qhd', weights, block_values)
            return (output, carried + lax.optimization_barrier(jnp.sum(fail_logs, axis=2)))
        zero_output = jnp.zeros((TOK_A, HEADS, HEAD_DIM), jnp.float32)
        zero_carried = jnp.zeros((HEADS, TOK_A), jnp.float32)
        output, unused = lax.fori_loop(0, own_block + 1, backward_turn, (zero_output, zero_carried))
        return output
    outputs = lax.map(one_shard, (query_split, jnp.arange(N_EP, dtype=jnp.int32)))
    return outputs.reshape(total_rows, HEADS * HEAD_DIM).astype(jnp.bfloat16)

def grouped_product(left_rows, right_matrix):
    part_width = left_rows.shape[1] // N_TP
    summed = jnp.zeros((left_rows.shape[0], right_matrix.shape[1]), jnp.float32)
    for part_index in range(N_TP):
        lower = part_index * part_width
        piece_sum = jnp.dot(left_rows[:, lower:lower + part_width], right_matrix[lower:lower + part_width], preferred_element_type=jnp.float32).astype(jnp.bfloat16)
        summed = summed + lax.optimization_barrier(piece_sum).astype(jnp.float32)
    return summed

def swiglu(chosen_rows, gate_weight, up_weight):
    gate_part = jnp.dot(chosen_rows, gate_weight, preferred_element_type=jnp.float32)
    up_part = jnp.dot(chosen_rows, up_weight, preferred_element_type=jnp.float32)
    return (jax.nn.silu(gate_part) * up_part).astype(jnp.bfloat16)

def routed_experts(normed, expert_index, route_weights, expert_gate, expert_up, expert_down):
    token_count = normed.shape[0]
    flat_expert = expert_index.reshape(-1).astype(jnp.int32)
    flat_token = jnp.repeat(jnp.arange(token_count, dtype=jnp.int32), TOPK)
    flat_weight = route_weights.reshape(-1)
    sort_order = jnp.argsort(flat_expert, stable=True)
    window = token_count // ROWS_B * CAP
    sorted_token = jnp.concatenate([flat_token[sort_order], jnp.zeros((window,), jnp.int32)])
    sorted_weight = jnp.concatenate([flat_weight[sort_order], jnp.zeros((window,), flat_weight.dtype)])
    counts = jax.ops.segment_sum(jnp.ones_like(flat_expert), flat_expert, EXPERTS).astype(jnp.int32)
    starts = (jnp.cumsum(counts) - counts).astype(jnp.int32)

    def one_expert(routed, expert_number):
        first_slot = starts[expert_number]
        tokens = lax.dynamic_slice_in_dim(sorted_token, first_slot, window)
        weights = lax.dynamic_slice_in_dim(sorted_weight, first_slot, window)
        live_slots = jnp.arange(window, dtype=jnp.int32) < counts[expert_number]
        chosen_rows = normed[tokens]
        hidden = swiglu(chosen_rows, expert_gate[expert_number], expert_up[expert_number])
        output = grouped_product(hidden, expert_down[expert_number]).astype(jnp.bfloat16)
        output = lax.optimization_barrier(output).astype(jnp.float32)
        return (routed.at[tokens].add(jnp.where(live_slots, weights, 0.0)[:, None] * output), None)
    routed, unused = lax.scan(one_expert, jnp.zeros((token_count, D), jnp.float32), jnp.arange(EXPERTS, dtype=jnp.int32))
    return routed

def reference(query_rows, key_rows, value_rows, key_bias, mixer_weight, mixer_gain, routed_input, entry_gain, expert_index, route_weights, expert_gate, expert_up, expert_down, shared_gate, shared_up, shared_down, exit_gain):
    attended = stick_breaking(query_rows, key_rows, value_rows, key_bias)
    mixer_sum = grouped_product(attended, mixer_weight)
    mixer_out = root_norm(mixer_sum, mixer_gain).astype(jnp.bfloat16)
    normed = root_norm(routed_input.astype(jnp.float32), entry_gain).astype(jnp.bfloat16)
    routed = routed_experts(normed, expert_index, route_weights, expert_gate, expert_up, expert_down)
    shared_hidden = swiglu(normed, shared_gate, shared_up)
    shared = grouped_product(shared_hidden, shared_down)
    expert_out = root_norm(routed + shared, exit_gain).astype(jnp.bfloat16)
    return (mixer_out, expert_out)
```

```python
import functools

import jax
import jax.numpy as jnp
from jax import lax
from jax.experimental import pallas as pl
from jax.experimental.pallas import tpu as pltpu
from jax.sharding import PartitionSpec as P

MESH = pl.DeviceIdType.MESH


def peer_places(ep_size, tp_size):
    own_ep = lax.axis_index("ep")
    own_tp = lax.axis_index("tp")
    partner = own_tp + 1 - 2 * lax.rem(own_tp, 2)
    across = lax.rem(own_tp + tp_size // 2, tp_size)
    return own_ep, own_tp, partner, across


def greet(ep_size, own_ep, own_tp, partner, across):
    barrier = pltpu.get_barrier_semaphore()

    def signal_one(step, unused):
        place = lax.rem(own_ep + step, ep_size)
        pl.semaphore_signal(barrier, inc=1, device_id=(place, own_tp), device_id_type=MESH)
        return unused

    lax.fori_loop(1, ep_size, signal_one, 0)
    for place in (partner, across):
        pl.semaphore_signal(barrier, inc=1, device_id=(own_ep, place), device_id_type=MESH)
    pl.semaphore_wait(barrier, ep_size + 1)


def send_of(source, target, send_sem, recv_sem, place):
    return pltpu.make_async_remote_copy(
        src_ref=source,
        dst_ref=target,
        send_sem=send_sem,
        recv_sem=recv_sem,
        device_id=place,
        device_id_type=MESH,
    )


def front_kernel(
    ep_size,
    tp_size,
    kv_ref,
    bias_ref,
    normed_ref,
    outgoing_ref,
    kv_all,
    bias_all,
    own_all,
    arrived,
    ep_send,
    ep_recv,
    kv_send,
    kv_recv,
    bias_send,
    bias_recv,
    partner_send,
    partner_recv,
    across_send,
    across_recv,
    relay_send,
    relay_recv,
    local_sem,
):
    own_ep, own_tp, partner, across = peer_places(ep_size, tp_size)
    greet(ep_size, own_ep, own_tp, partner, across)
    to_partner = (own_ep, partner)
    to_across = (own_ep, across)

    def dispatch(step):
        target = lax.rem(own_ep + step, ep_size)
        return send_of(
            outgoing_ref.at[target],
            arrived.at[own_tp, own_ep],
            ep_send.at[step],
            ep_recv.at[step],
            (target, own_tp),
        )

    def landed(step):
        source = lax.rem(own_ep - step + ep_size, ep_size)
        block = arrived.at[own_tp, source]
        return send_of(block, block, ep_send.at[step], ep_recv.at[step], (own_ep, own_tp))

    def spread_kv(step):
        target = lax.rem(own_ep + step, ep_size)
        return send_of(
            kv_ref, kv_all.at[own_ep], kv_send.at[step], kv_recv.at[step], (target, own_tp)
        )

    def landed_kv(step):
        block = kv_all.at[lax.rem(own_ep - step + ep_size, ep_size)]
        return send_of(block, block, kv_send.at[step], kv_recv.at[step], (own_ep, own_tp))

    def spread_bias(step):
        target = lax.rem(own_ep + step, ep_size)
        return send_of(
            bias_ref, bias_all.at[own_ep], bias_send.at[step], bias_recv.at[step], (target, own_tp)
        )

    def landed_bias(step):
        block = bias_all.at[lax.rem(own_ep - step + ep_size, ep_size)]
        return send_of(block, block, bias_send.at[step], bias_recv.at[step], (own_ep, own_tp))

    def tp_block(holder, step):
        return arrived.at[holder, lax.rem(own_ep - step + ep_size, ep_size)]

    def tp_copy(source, target, sems, step, place):
        return send_of(source, target, sems[0].at[step], sems[1].at[step], place)

    partner_sems = (partner_send, partner_recv)
    across_sems = (across_send, across_recv)
    relay_sems = (relay_send, relay_recv)
    last = ep_size

    lax.fori_loop(1, ep_size, lambda step, c: (dispatch(step).start(), c)[1], 0)
    own_block = outgoing_ref.at[own_ep]
    own_slot = arrived.at[own_tp, own_ep]
    tp_copy(normed_ref, own_all.at[own_tp], across_sems, last, to_across).start()
    tp_copy(own_block, own_slot, across_sems, 0, to_across).start()
    tp_copy(normed_ref, own_all.at[own_tp], partner_sems, last, to_partner).start()
    tp_copy(own_block, own_slot, partner_sems, 0, to_partner).start()
    locals_ = [
        pltpu.make_async_copy(own_block, own_slot, local_sem.at[0]),
        pltpu.make_async_copy(normed_ref, own_all.at[own_tp], local_sem.at[1]),
        pltpu.make_async_copy(kv_ref, kv_all.at[own_ep], local_sem.at[2]),
        pltpu.make_async_copy(bias_ref, bias_all.at[own_ep], local_sem.at[3]),
    ]
    for local in locals_:
        local.start()

    def start_kv(step, carry):
        spread_kv(step).start()
        spread_bias(step).start()
        return carry

    lax.fori_loop(1, ep_size, start_kv, 0)

    def forward(step, carry):
        landed(step).wait_recv()
        block = tp_block(own_tp, step)
        tp_copy(block, block, across_sems, step, to_across).start()
        tp_copy(block, block, partner_sems, step, to_partner).start()
        return carry

    lax.fori_loop(1, ep_size, forward, 0)

    other_own = own_all.at[across]
    tp_copy(other_own, other_own, across_sems, last, to_across).wait_recv()
    tp_copy(other_own, other_own, relay_sems, last, to_partner).start()

    def relay(step, carry):
        block = tp_block(across, step)
        tp_copy(block, block, across_sems, step, to_across).wait_recv()
        tp_copy(block, block, relay_sems, step, to_partner).start()
        return carry

    lax.fori_loop(0, ep_size, relay, 0)

    diagonal = lax.rem(partner + tp_size // 2, tp_size)

    def finish(step, carry):
        near = tp_block(partner, step)
        far = tp_block(diagonal, step)
        tp_copy(near, near, partner_sems, step, to_partner).wait()
        tp_copy(far, far, relay_sems, step, to_partner).wait()
        tp_copy(near, near, across_sems, step, to_across).wait_send()
        return carry

    lax.fori_loop(0, ep_size, finish, 0)
    near = own_all.at[partner]
    far = own_all.at[diagonal]
    tp_copy(near, near, partner_sems, last, to_partner).wait()
    tp_copy(far, far, relay_sems, last, to_partner).wait()
    tp_copy(near, near, across_sems, last, to_across).wait_send()

    def finish_ep(step, carry):
        dispatch(step).wait_send()
        spread_kv(step).wait_send()
        spread_bias(step).wait_send()
        landed_kv(step).wait_recv()
        landed_bias(step).wait_recv()
        return carry

    lax.fori_loop(1, ep_size, finish_ep, 0)
    for local in locals_:
        local.wait()


def front_exchange(ep_size, tp_size, kv, bias, normed, outgoing):
    def spread(count, value):
        return jax.ShapeDtypeStruct((count,) + value.shape, value.dtype)

    ep_sem = pltpu.SemaphoreType.DMA((ep_size,))
    tp_sem = pltpu.SemaphoreType.DMA((ep_size + 1,))
    return pl.pallas_call(
        functools.partial(front_kernel, ep_size, tp_size),
        out_shape=(
            spread(ep_size, kv),
            spread(ep_size, bias),
            spread(tp_size, normed),
            spread(tp_size, outgoing),
        ),
        in_specs=[pl.BlockSpec(memory_space=pltpu.VMEM)] * 4,
        out_specs=[pl.BlockSpec(memory_space=pl.ANY)] * 4,
        scratch_shapes=[ep_sem] * 6 + [tp_sem] * 6 + [pltpu.SemaphoreType.DMA((4,))],
        compiler_params=pltpu.CompilerParams(collective_id=0, has_side_effects=True),
        name="front_exchange",
    )(kv, bias, normed, outgoing)


def back_kernel(
    ep_size,
    tp_size,
    part_ref,
    shared_ref,
    mixer_ref,
    back_ref,
    shared_out,
    mixer_out,
    near_in,
    near_shared,
    near_mixer,
    far_out,
    far_in,
    far_shared_out,
    far_shared,
    far_mixer_out,
    far_mixer,
    total,
    near_send,
    near_recv,
    far_send,
    far_recv,
    ep_send,
    ep_recv,
    local_sem,
):
    own_ep, own_tp, partner, across = peer_places(ep_size, tp_size)
    diagonal = lax.rem(partner + tp_size // 2, tp_size)
    greet(ep_size, own_ep, own_tp, partner, across)
    to_partner = (own_ep, partner)
    to_across = (own_ep, across)
    homes = (diagonal, partner)

    def place_of(step):
        return lax.rem(own_ep + 1 + step, ep_size)

    def near_copy(side, step):
        place = place_of(step)
        return send_of(
            part_ref.at[homes[side], place],
            near_in.at[side, place],
            near_send.at[side, step],
            near_recv.at[side, step],
            to_partner,
        )

    def near_small(side, source, target, slot):
        return send_of(
            source.at[homes[side]],
            target.at[side],
            near_send.at[side, slot],
            near_recv.at[side, slot],
            to_partner,
        )

    def far_copy(source, target, slot):
        return send_of(source, target, far_send.at[slot], far_recv.at[slot], to_across)

    shared_slot, mixer_slot = ep_size, ep_size + 1

    for side in range(2):
        lax.fori_loop(
            0, ep_size, lambda step, c, side=side: (near_copy(side, step).start(), c)[1], 0
        )
        near_small(side, shared_ref, near_shared, shared_slot).start()
        near_small(side, mixer_ref, near_mixer, mixer_slot).start()

    def add(left, right):
        return left.astype(jnp.float32) + right.astype(jnp.float32)

    def pass_on(step, carry):
        place = place_of(step)
        near_copy(0, step).wait_recv()
        far_out[place] = add(part_ref[across, place], near_in[0, place]).astype(jnp.bfloat16)
        far_copy(far_out.at[place], far_in.at[place], step).start()
        return carry

    lax.fori_loop(0, ep_size, pass_on, 0)
    near_small(0, shared_ref, near_shared, shared_slot).wait_recv()
    far_shared_out[...] = add(shared_ref[across], near_shared[0]).astype(jnp.bfloat16)
    far_copy(far_shared_out, far_shared, shared_slot).start()
    near_small(0, mixer_ref, near_mixer, mixer_slot).wait_recv()
    far_mixer_out[...] = add(mixer_ref[across], near_mixer[0]).astype(jnp.bfloat16)
    far_copy(far_mixer_out, far_mixer, mixer_slot).start()

    def send_back(step):
        place = place_of(step)
        return send_of(
            total.at[place],
            back_ref.at[own_ep],
            ep_send.at[step],
            ep_recv.at[step],
            (place, own_tp),
        )

    def gather_total(step):
        place = place_of(step)
        near_copy(1, step).wait_recv()
        far_copy(far_out.at[place], far_in.at[place], step).wait_recv()
        value = add(part_ref[own_tp, place], near_in[1, place]) + far_in[place].astype(jnp.float32)
        total[place] = value.astype(jnp.bfloat16)

    def return_one(step, carry):
        gather_total(step)
        send_back(step).start()
        return carry

    lax.fori_loop(0, ep_size - 1, return_one, 0)
    gather_total(ep_size - 1)
    local = pltpu.make_async_copy(total.at[own_ep], back_ref.at[own_ep], local_sem)
    local.start()

    near_small(1, shared_ref, near_shared, shared_slot).wait_recv()
    far_copy(far_shared_out, far_shared, shared_slot).wait_recv()
    shared_out[...] = add(shared_ref[own_tp], near_shared[1]) + far_shared[...].astype(jnp.float32)
    near_small(1, mixer_ref, near_mixer, mixer_slot).wait_recv()
    far_copy(far_mixer_out, far_mixer, mixer_slot).wait_recv()
    mixer_out[...] = add(mixer_ref[own_tp], near_mixer[1]) + far_mixer[...].astype(jnp.float32)

    def finish(step, carry):
        place = place_of(step)
        near_copy(0, step).wait_send()
        near_copy(1, step).wait_send()
        far_copy(far_out.at[place], far_in.at[place], step).wait_send()
        return carry

    lax.fori_loop(0, ep_size, finish, 0)
    for side in range(2):
        near_small(side, shared_ref, near_shared, shared_slot).wait_send()
        near_small(side, mixer_ref, near_mixer, mixer_slot).wait_send()
    far_copy(far_shared_out, far_shared, shared_slot).wait_send()
    far_copy(far_mixer_out, far_mixer, mixer_slot).wait_send()

    def finish_ep(step, carry):
        send_back(step).wait_send()
        source = lax.rem(own_ep - 1 - step + 2 * ep_size, ep_size)
        block = back_ref.at[source]
        send_of(
            block, block, ep_send.at[step], ep_recv.at[step], (own_ep, own_tp)
        ).wait_recv()
        return carry

    lax.fori_loop(0, ep_size - 1, finish_ep, 0)
    local.wait()


def back_exchange(ep_size, tp_size, part, shared, mixer):
    block = part.shape[2:]
    bf16 = jnp.bfloat16
    sem = pltpu.SemaphoreType.DMA
    vmem = pl.BlockSpec(memory_space=pltpu.VMEM)
    return pl.pallas_call(
        functools.partial(back_kernel, ep_size, tp_size),
        out_shape=(
            jax.ShapeDtypeStruct((ep_size,) + block, bf16),
            jax.ShapeDtypeStruct(shared.shape[1:], jnp.float32),
            jax.ShapeDtypeStruct(mixer.shape[1:], jnp.float32),
        ),
        in_specs=[vmem] * 3,
        out_specs=[pl.BlockSpec(memory_space=pl.ANY), vmem, vmem],
        scratch_shapes=[
            pltpu.VMEM((2, ep_size) + block, bf16),
            pltpu.VMEM((2,) + shared.shape[1:], bf16),
            pltpu.VMEM((2,) + mixer.shape[1:], bf16),
            pltpu.VMEM((ep_size,) + block, bf16),
            pltpu.VMEM((ep_size,) + block, bf16),
            pltpu.VMEM(shared.shape[1:], bf16),
            pltpu.VMEM(shared.shape[1:], bf16),
            pltpu.VMEM(mixer.shape[1:], bf16),
            pltpu.VMEM(mixer.shape[1:], bf16),
            pltpu.VMEM((ep_size,) + block, bf16),
            sem((2, ep_size + 2)),
            sem((2, ep_size + 2)),
            sem((ep_size + 2,)),
            sem((ep_size + 2,)),
            sem((ep_size,)),
            sem((ep_size,)),
            sem,
        ],
        compiler_params=pltpu.CompilerParams(
            collective_id=1, has_side_effects=True, vmem_limit_bytes=60 * 1024 * 1024
        ),
        name="back_exchange",
    )(part, shared, mixer)


EPS = 1e-06


def root_norm(values, gain_row):
    return values * lax.rsqrt(jnp.mean(values * values, axis=-1, keepdims=True) + EPS) * gain_row


def block_shards(shard_rows, ep_size):
    shards = 1
    while shards * shard_rows < 512 and ep_size % (2 * shards) == 0:
        shards = shards * 2
    return shards


def break_scores(query_split, block_keys, block_bias, query_pos, key_start):
    head_count = query_split.shape[1]
    key_count = block_keys.shape[0]
    keys_split = block_keys.reshape(key_count, head_count, query_split.shape[2])
    scores = jnp.einsum("qhd,khd->hqk", query_split, keys_split, preferred_element_type=jnp.float32)
    scores = (
        scores * query_split.shape[2] ** (-0.5)
        + jnp.transpose(block_bias.astype(jnp.float32))[:, None, :]
    )
    key_pos = key_start + jnp.arange(key_count, dtype=jnp.int32)
    causal = (key_pos[None, :] < query_pos[:, None])[None]
    fail_logs = jnp.where(causal, -jax.nn.softplus(scores), 0.0)
    return (scores, fail_logs, causal)


def break_values(scores, fail_logs, causal, offset, block_values):
    later_sum = lax.cumsum(fail_logs, axis=2, reverse=True) - fail_logs + offset[:, :, None]
    weights = jnp.where(causal, jnp.exp(jax.nn.log_sigmoid(scores) + later_sum), 0.0).astype(
        jnp.bfloat16
    )
    values_split = block_values.reshape(block_values.shape[0], scores.shape[0], -1)
    return jnp.einsum("hqk,khd->qhd", weights, values_split, preferred_element_type=jnp.float32)


def shared_term_of(own_all, shared_gate, shared_up, shared_down):
    gate_part = jnp.dot(own_all, shared_gate, preferred_element_type=jnp.float32)
    up_part = jnp.dot(own_all, shared_up, preferred_element_type=jnp.float32)
    hidden = (jax.nn.silu(gate_part) * up_part).astype(jnp.bfloat16)
    return jnp.dot(hidden, shared_down, preferred_element_type=jnp.float32).astype(jnp.bfloat16)


def on_device(
    query_rows,
    key_rows,
    value_rows,
    key_bias,
    mixer_weight,
    mixer_gain,
    routed_input,
    entry_gain,
    expert_index,
    route_weights,
    expert_gate,
    expert_up,
    expert_down,
    shared_gate,
    shared_up,
    shared_down,
    exit_gain,
):
    shard_rows = query_rows.shape[0]
    head_count = key_bias.shape[1]
    head_size = query_rows.shape[1] // head_count
    ep_size = lax.axis_size("ep")
    tp_size = lax.axis_size("tp")
    own_index = lax.axis_index("ep")
    query_split = query_rows.reshape(shard_rows, head_count, head_size)
    query_pos = own_index * shard_rows + jnp.arange(shard_rows, dtype=jnp.int32)
    span_shards = block_shards(shard_rows, ep_size)
    empty_output = jnp.zeros((shard_rows, head_count, head_size), jnp.float32)
    row_count = routed_input.shape[0]
    local_experts = expert_gate.shape[0]
    model_width = routed_input.shape[1]
    expert_count = local_experts * ep_size
    top_count = expert_index.shape[1]
    capacity = 3 * row_count * top_count // (2 * expert_count)
    block_slots = -(-local_experts * capacity // 16) * 16
    slot_total = ep_size * block_slots
    normed = root_norm(routed_input.astype(jnp.float32), entry_gain).astype(jnp.bfloat16)
    flat_expert = expert_index.reshape(-1)
    onehot = (flat_expert[:, None] == jnp.arange(expert_count, dtype=jnp.int32)[None, :]).astype(
        jnp.int32
    )
    slot_rank = jnp.sum((jnp.cumsum(onehot, axis=0) - onehot) * onehot, axis=1)
    slot_index = (
        flat_expert // local_experts * block_slots
        + flat_expert % local_experts * capacity
        + slot_rank
    ).reshape(row_count, top_count)
    slots = jnp.arange(slot_total, dtype=jnp.int32)
    matches = slot_index[None, :, :] == slots[:, None, None]
    selector = jnp.any(matches, axis=2).astype(jnp.bfloat16)
    outgoing = jnp.dot(selector, normed, preferred_element_type=jnp.float32).astype(jnp.bfloat16)
    outgoing = outgoing.reshape(ep_size, block_slots, model_width)
    bias_rows = -(-head_count // 16) * 16
    bias_block = jnp.pad(jnp.transpose(key_bias), ((0, bias_rows - head_count), (0, 0)))
    kv_block = jnp.concatenate([key_rows, value_rows], axis=1)
    kv_all, bias_all, own_all, arrived = front_exchange(
        ep_size, tp_size, kv_block, bias_block, normed, outgoing
    )
    width = key_rows.shape[1]
    all_keys = kv_all[:, :, :width].reshape(ep_size * shard_rows, width)
    all_values = kv_all[:, :, width:].reshape(ep_size * shard_rows, width)
    all_bias = jnp.swapaxes(bias_all[:, :head_count, :], 1, 2).reshape(
        ep_size * shard_rows, head_count
    )
    own_all = own_all.reshape(tp_size * row_count, model_width)
    block_rows = span_shards * shard_rows
    own_block = own_index * shard_rows // block_rows

    def backward_turn(turn_index, carried_pair):
        output, carried = carried_pair
        block_start = (own_block - turn_index) * block_rows
        block_keys = lax.dynamic_slice_in_dim(all_keys, block_start, block_rows, 0)
        block_values = lax.dynamic_slice_in_dim(all_values, block_start, block_rows, 0)
        block_bias = lax.dynamic_slice_in_dim(all_bias, block_start, block_rows, 0)
        scores, fail_logs, causal = break_scores(
            query_split, block_keys, block_bias, query_pos, block_start
        )
        output = output + break_values(scores, fail_logs, causal, carried, block_values)
        return (output, carried + jnp.sum(fail_logs, axis=2))

    carried_zero = jnp.zeros((head_count, shard_rows), jnp.float32)
    output, unused = lax.fori_loop(0, own_block + 1, backward_turn, (empty_output, carried_zero))
    attended = output.reshape(shard_rows, head_count * head_size).astype(jnp.bfloat16)
    mixer_term = jnp.dot(attended, mixer_weight, preferred_element_type=jnp.float32).astype(
        jnp.bfloat16
    )
    rows = arrived.reshape(tp_size * slot_total, model_width)
    row_expert = jnp.arange(tp_size * slot_total, dtype=jnp.int32) % block_slots // capacity
    pieces = []
    for expert in range(local_experts):
        gate_part = jnp.dot(rows, expert_gate[expert], preferred_element_type=jnp.float32)
        up_part = jnp.dot(rows, expert_up[expert], preferred_element_type=jnp.float32)
        hidden = jax.nn.silu(gate_part) * up_part
        pieces.append(jnp.where((row_expert == expert)[:, None], hidden, 0.0).astype(jnp.bfloat16))
    hidden = jnp.concatenate(pieces, axis=1)
    down = expert_down.reshape(hidden.shape[1], model_width)
    part = jnp.dot(hidden, down, preferred_element_type=jnp.float32).astype(jnp.bfloat16)
    part = part.reshape(tp_size, ep_size, block_slots, model_width)
    shared_term = shared_term_of(own_all, shared_gate, shared_up, shared_down).reshape(
        tp_size, row_count, model_width
    )
    mixer_term = mixer_term.reshape(tp_size, shard_rows // tp_size, model_width)
    back_rows, shared_sum, mixer_sum = back_exchange(
        ep_size, tp_size, part, shared_term, mixer_term
    )
    back_rows = back_rows.reshape(slot_total, model_width)
    placed = slot_index[:, :, None] == slots[None, None, :]
    mixing = jnp.sum(jnp.where(placed, route_weights[:, :, None], 0.0), axis=1)
    mixing_high = mixing.astype(jnp.bfloat16)
    mixing_low = (mixing - mixing_high.astype(jnp.float32)).astype(jnp.bfloat16)
    routed = jnp.dot(mixing_high, back_rows, preferred_element_type=jnp.float32) + jnp.dot(
        mixing_low, back_rows, preferred_element_type=jnp.float32
    )
    combined = routed + shared_sum
    expert_out = root_norm(combined, exit_gain).astype(jnp.bfloat16)
    mixer_out = root_norm(mixer_sum, mixer_gain).astype(jnp.bfloat16)
    return (mixer_out, expert_out)


def solution(mesh):
    in_specs = (
        P("ep", "tp"),
        P("ep", "tp"),
        P("ep", "tp"),
        P("ep", "tp"),
        P("tp", None),
        P(),
        P(("ep", "tp"), None),
        P(),
        P(("ep", "tp"), None),
        P(("ep", "tp"), None),
        P("ep", None, "tp"),
        P("ep", None, "tp"),
        P("ep", "tp", None),
        P(None, "tp"),
        P(None, "tp"),
        P("tp", None),
        P(),
    )
    out_specs = (P(("ep", "tp"), None), P(("ep", "tp"), None))
    return jax.shard_map(
        on_device, mesh=mesh, in_specs=in_specs, out_specs=out_specs, check_vma=False
    )
```

```python
import functools

import jax
import jax.numpy as jnp
from jax import lax
from jax.experimental import pallas as pl
from jax.experimental.pallas import tpu as pltpu
from jax.sharding import PartitionSpec as P

MESH = pl.DeviceIdType.MESH


def peer_places(ep_size, tp_size):
    own_ep = lax.axis_index("ep")
    own_tp = lax.axis_index("tp")
    partner = own_tp + 1 - 2 * lax.rem(own_tp, 2)
    across = lax.rem(own_tp + tp_size // 2, tp_size)
    return own_ep, own_tp, partner, across


def greet(ep_size, own_ep, own_tp, partner, across):
    barrier = pltpu.get_barrier_semaphore()

    def signal_one(step, unused):
        place = lax.rem(own_ep + step, ep_size)
        pl.semaphore_signal(barrier, inc=1, device_id=(place, own_tp), device_id_type=MESH)
        return unused

    lax.fori_loop(1, ep_size, signal_one, 0)
    for place in (partner, across):
        pl.semaphore_signal(barrier, inc=1, device_id=(own_ep, place), device_id_type=MESH)
    pl.semaphore_wait(barrier, ep_size + 1)


def send_of(source, target, send_sem, recv_sem, place):
    return pltpu.make_async_remote_copy(
        src_ref=source,
        dst_ref=target,
        send_sem=send_sem,
        recv_sem=recv_sem,
        device_id=place,
        device_id_type=MESH,
    )


def front_kernel(
    ep_size,
    tp_size,
    head_size,
    query_ref,
    kv_ref,
    normed_ref,
    outgoing_ref,
    attended_ref,
    own_all,
    arrived,
    kv_all,
    query_heads,
    carried,
    output,
    ep_send,
    ep_recv,
    kv_send,
    kv_recv,
    pair_send,
    pair_recv,
    partner_send,
    partner_recv,
    across_send,
    across_recv,
    relay_send,
    relay_recv,
    local_sem,
):
    own_ep, own_tp, partner, across = peer_places(ep_size, tp_size)
    greet(ep_size, own_ep, own_tp, partner, across)
    to_partner = (own_ep, partner)
    to_across = (own_ep, across)

    def dispatch(step):
        target = lax.rem(own_ep + step, ep_size)
        return send_of(
            outgoing_ref.at[target],
            arrived.at[own_tp, own_ep],
            ep_send.at[step],
            ep_recv.at[step],
            (target, own_tp),
        )

    def landed(step):
        source = lax.rem(own_ep - step + ep_size, ep_size)
        block = arrived.at[own_tp, source]
        return send_of(block, block, ep_send.at[step], ep_recv.at[step], (own_ep, own_tp))

    shard_rows, width = query_ref.shape
    head_count = width // head_size
    lines = ep_size // 2
    parity = lax.rem(own_ep, 2)
    own_line = own_ep // 2
    pair_ep = own_ep + 1 - 2 * parity

    def spread_kv(step):
        target = 2 * lax.rem(own_line + step, lines) + parity
        return send_of(
            kv_ref, kv_all.at[own_ep], kv_send.at[step], kv_recv.at[step], (target, own_tp)
        )

    def line_kv(step, side):
        return kv_all.at[2 * lax.rem(own_line - step + lines, lines) + side]

    def landed_kv(step):
        block = line_kv(step, parity)
        return send_of(block, block, kv_send.at[step], kv_recv.at[step], (own_ep, own_tp))

    def pair_kv(source, target, step):
        return send_of(
            source, target, pair_send.at[step], pair_recv.at[step], (pair_ep, own_tp)
        )

    def attend_block(keys_values, own):
        keys = keys_values[0:shard_rows, 0:width]
        values = keys_values[0:shard_rows, width : 2 * width]
        ahead = lax.broadcasted_iota(jnp.int32, (shard_rows, shard_rows), 0)
        behind = lax.broadcasted_iota(jnp.int32, (shard_rows, shard_rows), 1)
        later_of = jnp.where(ahead > behind, 1.0, 0.0)
        column_head = lax.broadcasted_iota(jnp.int32, (shard_rows, width), 1) // head_size
        gained = jnp.zeros((shard_rows, width), jnp.float32)
        for head in range(head_count):
            bias_row = keys_values[shard_rows + head : shard_rows + head + 1, 0:shard_rows]
            scores = lax.dot_general(
                query_heads[head],
                keys,
                (((1,), (1,)), ((), ())),
                preferred_element_type=jnp.float32,
            )
            scores = scores * head_size ** (-0.5) + bias_row.astype(jnp.float32)
            tail = jnp.log1p(jnp.exp(-jnp.abs(scores)))
            fails = -(jnp.maximum(scores, 0.0) + tail)
            if own:
                fails = jnp.where(behind < ahead, fails, 0.0)
            later = jnp.dot(
                fails,
                later_of,
                preferred_element_type=jnp.float32,
                precision=lax.Precision.HIGHEST,
            )
            weights = jnp.exp(jnp.minimum(scores, 0.0) - tail + later + carried[head])
            if own:
                weights = jnp.where(behind < ahead, weights, 0.0)
            product = jnp.dot(
                weights.astype(jnp.bfloat16), values, preferred_element_type=jnp.float32
            )
            gained = jnp.where(column_head == head, product, gained)
            carried[head] = carried[head] + jnp.sum(fails, axis=1, keepdims=True)
        output[...] = output[...] + gained

    def tp_block(holder, step):
        return arrived.at[holder, lax.rem(own_ep - step + ep_size, ep_size)]

    def tp_copy(source, target, sems, step, place):
        return send_of(source, target, sems[0].at[step], sems[1].at[step], place)

    partner_sems = (partner_send, partner_recv)
    across_sems = (across_send, across_recv)
    relay_sems = (relay_send, relay_recv)
    last = ep_size

    lax.fori_loop(1, lines, lambda step, c: (spread_kv(step).start(), c)[1], 0)
    pair_kv(kv_ref, kv_all.at[own_ep], 0).start()
    lax.fori_loop(1, ep_size, lambda step, c: (dispatch(step).start(), c)[1], 0)
    own_block = outgoing_ref.at[own_ep]
    own_slot = arrived.at[own_tp, own_ep]
    tp_copy(normed_ref, own_all.at[own_tp], across_sems, last, to_across).start()
    tp_copy(own_block, own_slot, across_sems, 0, to_across).start()
    tp_copy(normed_ref, own_all.at[own_tp], partner_sems, last, to_partner).start()
    tp_copy(own_block, own_slot, partner_sems, 0, to_partner).start()
    locals_ = [
        pltpu.make_async_copy(own_block, own_slot, local_sem.at[0]),
        pltpu.make_async_copy(normed_ref, own_all.at[own_tp], local_sem.at[1]),
    ]
    for local in locals_:
        local.start()

    output[...] = jnp.zeros_like(output)
    carried[...] = jnp.zeros_like(carried)
    head_of = lax.broadcasted_iota(jnp.int32, (shard_rows, width), 1) // head_size
    queries = query_ref[...].astype(jnp.float32)
    for head in range(head_count):
        query_heads[head] = jnp.where(head_of == head, queries, 0.0).astype(jnp.bfloat16)
    attend_block(kv_ref[...], True)

    def relay_kv(step, carry):
        landed_kv(step).wait_recv()
        block = line_kv(step, parity)
        pair_kv(block, block, step).start()
        return carry

    lax.fori_loop(1, lines, relay_kv, 0)

    def landed_pair(step, carry):
        block = line_kv(step, 1 - parity)
        pair_kv(block, block, step).wait_recv()
        return carry

    lax.fori_loop(0, lines, landed_pair, 0)

    def forward(step, carry):
        landed(step).wait_recv()
        block = tp_block(own_tp, step)
        tp_copy(block, block, across_sems, step, to_across).start()
        tp_copy(block, block, partner_sems, step, to_partner).start()

        @pl.when(step <= own_ep)
        def attend_earlier():
            attend_block(kv_all[lax.rem(own_ep - step + ep_size, ep_size)], False)

        return carry

    lax.fori_loop(1, ep_size, forward, 0)
    attended_ref[...] = output[...].astype(jnp.bfloat16)

    other_own = own_all.at[across]
    tp_copy(other_own, other_own, across_sems, last, to_across).wait_recv()
    tp_copy(other_own, other_own, relay_sems, last, to_partner).start()

    def relay(step, carry):
        block = tp_block(across, step)
        tp_copy(block, block, across_sems, step, to_across).wait_recv()
        tp_copy(block, block, relay_sems, step, to_partner).start()
        return carry

    lax.fori_loop(0, ep_size, relay, 0)

    diagonal = lax.rem(partner + tp_size // 2, tp_size)

    def finish(step, carry):
        near = tp_block(partner, step)
        far = tp_block(diagonal, step)
        tp_copy(near, near, partner_sems, step, to_partner).wait()
        tp_copy(far, far, relay_sems, step, to_partner).wait()
        tp_copy(near, near, across_sems, step, to_across).wait_send()
        return carry

    lax.fori_loop(0, ep_size, finish, 0)
    near = own_all.at[partner]
    far = own_all.at[diagonal]
    tp_copy(near, near, partner_sems, last, to_partner).wait()
    tp_copy(far, far, relay_sems, last, to_partner).wait()
    tp_copy(near, near, across_sems, last, to_across).wait_send()

    def finish_ep(step, carry):
        dispatch(step).wait_send()
        return carry

    lax.fori_loop(1, ep_size, finish_ep, 0)

    def finish_kv(step, carry):
        block = line_kv(step, parity)
        pair_kv(block, block, step).wait_send()
        return carry

    lax.fori_loop(1, lines, finish_kv, 0)
    lax.fori_loop(1, lines, lambda step, c: (spread_kv(step).wait_send(), c)[1], 0)
    pair_kv(kv_ref, kv_all.at[own_ep], 0).wait_send()
    for local in locals_:
        local.wait()


def front_exchange(ep_size, tp_size, head_size, queries, kv, normed, outgoing):
    def spread(count, value):
        return jax.ShapeDtypeStruct((count,) + value.shape, value.dtype)

    rows, width = queries.shape
    heads = width // head_size
    ep_sem = pltpu.SemaphoreType.DMA((ep_size,))
    tp_sem = pltpu.SemaphoreType.DMA((ep_size + 1,))
    vmem = pl.BlockSpec(memory_space=pltpu.VMEM)
    return pl.pallas_call(
        functools.partial(front_kernel, ep_size, tp_size, head_size),
        out_shape=(
            jax.ShapeDtypeStruct(queries.shape, jnp.bfloat16),
            spread(tp_size, normed),
            spread(tp_size, outgoing),
        ),
        in_specs=[vmem] * 4,
        out_specs=[vmem] + [pl.BlockSpec(memory_space=pl.ANY)] * 2,
        scratch_shapes=[
            pltpu.VMEM((ep_size,) + kv.shape, kv.dtype),
            pltpu.VMEM((heads, rows, width), jnp.bfloat16),
            pltpu.VMEM((heads, rows, 1), jnp.float32),
            pltpu.VMEM((rows, width), jnp.float32),
        ]
        + [ep_sem] * 6
        + [tp_sem] * 6
        + [pltpu.SemaphoreType.DMA((2,))],
        compiler_params=pltpu.CompilerParams(
            collective_id=0, has_side_effects=True, vmem_limit_bytes=48 * 1024 * 1024
        ),
        name="front_exchange",
    )(queries, kv, normed, outgoing)


def expert_kernel(capacity, block_slots, rows_ref, gate_ref, up_ref, down_ref, part_ref):
    rows = rows_ref[...]
    row_expert = (
        lax.rem(lax.broadcasted_iota(jnp.int32, (rows.shape[0], 1), 0), block_slots) // capacity
    )
    total = jnp.zeros(part_ref.shape, jnp.float32)
    for expert in range(gate_ref.shape[0]):
        gate = jnp.dot(rows, gate_ref[expert], preferred_element_type=jnp.float32)
        up = jnp.dot(rows, up_ref[expert], preferred_element_type=jnp.float32)
        hidden = gate / (1.0 + jnp.exp(-gate)) * up
        hidden = jnp.where(row_expert == expert, hidden, 0.0).astype(jnp.bfloat16)
        total = total + jnp.dot(hidden, down_ref[expert], preferred_element_type=jnp.float32)
    part_ref[...] = total.astype(jnp.bfloat16)


def expert_parts(capacity, block_slots, tile, rows, gate, up, down):
    row_total, width = rows.shape

    def whole(value):
        return pl.BlockSpec(value.shape, lambda i: (0, 0, 0))

    return pl.pallas_call(
        functools.partial(expert_kernel, capacity, block_slots),
        grid=(row_total // tile,),
        out_shape=jax.ShapeDtypeStruct((row_total, width), jnp.bfloat16),
        in_specs=[pl.BlockSpec((tile, width), lambda i: (i, 0)), whole(gate), whole(up), whole(down)],
        out_specs=pl.BlockSpec((tile, width), lambda i: (i, 0)),
        compiler_params=pltpu.CompilerParams(vmem_limit_bytes=60 * 1024 * 1024),
        name="expert_parts",
    )(rows, gate, up, down)


def back_kernel(
    ep_size,
    tp_size,
    part_ref,
    shared_ref,
    mixer_ref,
    back_ref,
    shared_out,
    mixer_out,
    near_in,
    near_shared,
    near_mixer,
    far_out,
    far_in,
    far_shared_out,
    far_shared,
    far_mixer_out,
    far_mixer,
    total,
    near_send,
    near_recv,
    far_send,
    far_recv,
    ep_send,
    ep_recv,
    local_sem,
):
    own_ep, own_tp, partner, across = peer_places(ep_size, tp_size)
    diagonal = lax.rem(partner + tp_size // 2, tp_size)
    greet(ep_size, own_ep, own_tp, partner, across)
    to_partner = (own_ep, partner)
    to_across = (own_ep, across)
    homes = (diagonal, partner)

    def place_of(step):
        return lax.rem(own_ep + 1 + step, ep_size)

    def near_copy(side, step):
        place = place_of(step)
        return send_of(
            part_ref.at[homes[side], place],
            near_in.at[side, place],
            near_send.at[side, step],
            near_recv.at[side, step],
            to_partner,
        )

    def near_small(side, source, target, slot):
        return send_of(
            source.at[homes[side]],
            target.at[side],
            near_send.at[side, slot],
            near_recv.at[side, slot],
            to_partner,
        )

    def far_copy(source, target, slot):
        return send_of(source, target, far_send.at[slot], far_recv.at[slot], to_across)

    shared_slot, mixer_slot = ep_size, ep_size + 1

    for side in range(2):
        lax.fori_loop(
            0, ep_size, lambda step, c, side=side: (near_copy(side, step).start(), c)[1], 0
        )
        near_small(side, shared_ref, near_shared, shared_slot).start()
        near_small(side, mixer_ref, near_mixer, mixer_slot).start()

    def add(left, right):
        return left.astype(jnp.float32) + right.astype(jnp.float32)

    def pass_on(step, carry):
        place = place_of(step)
        near_copy(0, step).wait_recv()
        far_out[place] = add(part_ref[across, place], near_in[0, place]).astype(jnp.bfloat16)
        far_copy(far_out.at[place], far_in.at[place], step).start()
        return carry

    lax.fori_loop(0, ep_size, pass_on, 0)
    near_small(0, shared_ref, near_shared, shared_slot).wait_recv()
    far_shared_out[...] = add(shared_ref[across], near_shared[0]).astype(jnp.bfloat16)
    far_copy(far_shared_out, far_shared, shared_slot).start()
    near_small(0, mixer_ref, near_mixer, mixer_slot).wait_recv()
    far_mixer_out[...] = add(mixer_ref[across], near_mixer[0]).astype(jnp.bfloat16)
    far_copy(far_mixer_out, far_mixer, mixer_slot).start()

    def send_back(step):
        place = place_of(step)
        return send_of(
            total.at[place],
            back_ref.at[own_ep],
            ep_send.at[step],
            ep_recv.at[step],
            (place, own_tp),
        )

    def gather_total(step):
        place = place_of(step)
        near_copy(1, step).wait_recv()
        far_copy(far_out.at[place], far_in.at[place], step).wait_recv()
        value = add(part_ref[own_tp, place], near_in[1, place]) + far_in[place].astype(jnp.float32)
        total[place] = value.astype(jnp.bfloat16)

    def return_one(step, carry):
        gather_total(step)
        send_back(step).start()
        return carry

    lax.fori_loop(0, ep_size - 1, return_one, 0)
    gather_total(ep_size - 1)
    local = pltpu.make_async_copy(total.at[own_ep], back_ref.at[own_ep], local_sem)
    local.start()

    near_small(1, shared_ref, near_shared, shared_slot).wait_recv()
    far_copy(far_shared_out, far_shared, shared_slot).wait_recv()
    shared_out[...] = add(shared_ref[own_tp], near_shared[1]) + far_shared[...].astype(jnp.float32)
    near_small(1, mixer_ref, near_mixer, mixer_slot).wait_recv()
    far_copy(far_mixer_out, far_mixer, mixer_slot).wait_recv()
    mixer_out[...] = add(mixer_ref[own_tp], near_mixer[1]) + far_mixer[...].astype(jnp.float32)

    def finish(step, carry):
        place = place_of(step)
        near_copy(0, step).wait_send()
        near_copy(1, step).wait_send()
        far_copy(far_out.at[place], far_in.at[place], step).wait_send()
        return carry

    lax.fori_loop(0, ep_size, finish, 0)
    for side in range(2):
        near_small(side, shared_ref, near_shared, shared_slot).wait_send()
        near_small(side, mixer_ref, near_mixer, mixer_slot).wait_send()
    far_copy(far_shared_out, far_shared, shared_slot).wait_send()
    far_copy(far_mixer_out, far_mixer, mixer_slot).wait_send()

    def finish_ep(step, carry):
        send_back(step).wait_send()
        source = lax.rem(own_ep - 1 - step + 2 * ep_size, ep_size)
        block = back_ref.at[source]
        send_of(
            block, block, ep_send.at[step], ep_recv.at[step], (own_ep, own_tp)
        ).wait_recv()
        return carry

    lax.fori_loop(0, ep_size - 1, finish_ep, 0)
    local.wait()


def back_exchange(ep_size, tp_size, part, shared, mixer):
    block = part.shape[2:]
    bf16 = jnp.bfloat16
    sem = pltpu.SemaphoreType.DMA
    vmem = pl.BlockSpec(memory_space=pltpu.VMEM)
    return pl.pallas_call(
        functools.partial(back_kernel, ep_size, tp_size),
        out_shape=(
            jax.ShapeDtypeStruct((ep_size,) + block, bf16),
            jax.ShapeDtypeStruct(shared.shape[1:], jnp.float32),
            jax.ShapeDtypeStruct(mixer.shape[1:], jnp.float32),
        ),
        in_specs=[vmem] * 3,
        out_specs=[pl.BlockSpec(memory_space=pl.ANY), vmem, vmem],
        scratch_shapes=[
            pltpu.VMEM((2, ep_size) + block, bf16),
            pltpu.VMEM((2,) + shared.shape[1:], bf16),
            pltpu.VMEM((2,) + mixer.shape[1:], bf16),
            pltpu.VMEM((ep_size,) + block, bf16),
            pltpu.VMEM((ep_size,) + block, bf16),
            pltpu.VMEM(shared.shape[1:], bf16),
            pltpu.VMEM(shared.shape[1:], bf16),
            pltpu.VMEM(mixer.shape[1:], bf16),
            pltpu.VMEM(mixer.shape[1:], bf16),
            pltpu.VMEM((ep_size,) + block, bf16),
            sem((2, ep_size + 2)),
            sem((2, ep_size + 2)),
            sem((ep_size + 2,)),
            sem((ep_size + 2,)),
            sem((ep_size,)),
            sem((ep_size,)),
            sem,
        ],
        compiler_params=pltpu.CompilerParams(
            collective_id=1, has_side_effects=True, vmem_limit_bytes=60 * 1024 * 1024
        ),
        name="back_exchange",
    )(part, shared, mixer)


EPS = 1e-06


def root_norm(values, gain_row):
    return values * lax.rsqrt(jnp.mean(values * values, axis=-1, keepdims=True) + EPS) * gain_row


def shared_term_of(own_all, shared_gate, shared_up, shared_down):
    gate_part = jnp.dot(own_all, shared_gate, preferred_element_type=jnp.float32)
    up_part = jnp.dot(own_all, shared_up, preferred_element_type=jnp.float32)
    hidden = (jax.nn.silu(gate_part) * up_part).astype(jnp.bfloat16)
    return jnp.dot(hidden, shared_down, preferred_element_type=jnp.float32).astype(jnp.bfloat16)


def on_device(
    query_rows,
    key_rows,
    value_rows,
    key_bias,
    mixer_weight,
    mixer_gain,
    routed_input,
    entry_gain,
    expert_index,
    route_weights,
    expert_gate,
    expert_up,
    expert_down,
    shared_gate,
    shared_up,
    shared_down,
    exit_gain,
):
    shard_rows = query_rows.shape[0]
    head_count = key_bias.shape[1]
    head_size = query_rows.shape[1] // head_count
    ep_size = lax.axis_size("ep")
    tp_size = lax.axis_size("tp")
    row_count = routed_input.shape[0]
    local_experts = expert_gate.shape[0]
    model_width = routed_input.shape[1]
    expert_count = local_experts * ep_size
    top_count = expert_index.shape[1]
    capacity = 3 * row_count * top_count // (2 * expert_count)
    block_slots = -(-local_experts * capacity // 8) * 8
    slot_total = ep_size * block_slots
    normed = root_norm(routed_input.astype(jnp.float32), entry_gain).astype(jnp.bfloat16)
    flat_expert = expert_index.reshape(-1)
    onehot = (flat_expert[:, None] == jnp.arange(expert_count, dtype=jnp.int32)[None, :]).astype(
        jnp.int32
    )
    slot_rank = jnp.sum((jnp.cumsum(onehot, axis=0) - onehot) * onehot, axis=1)
    slot_index = (
        flat_expert // local_experts * block_slots
        + flat_expert % local_experts * capacity
        + slot_rank
    ).reshape(row_count, top_count)
    slots = jnp.arange(slot_total, dtype=jnp.int32)
    matches = slot_index[None, :, :] == slots[:, None, None]
    selector = jnp.any(matches, axis=2).astype(jnp.bfloat16)
    outgoing = jnp.dot(selector, normed, preferred_element_type=jnp.float32).astype(jnp.bfloat16)
    outgoing = outgoing.reshape(ep_size, block_slots, model_width)
    bias_rows = -(-head_count // 16) * 16
    bias_block = jnp.pad(
        jnp.transpose(key_bias),
        ((0, bias_rows - head_count), (0, 2 * key_rows.shape[1] - shard_rows)),
    )
    kv_block = jnp.concatenate(
        [jnp.concatenate([key_rows, value_rows], axis=1), bias_block], axis=0
    )
    attended, own_all, arrived = front_exchange(
        ep_size, tp_size, head_size, query_rows, kv_block, normed, outgoing
    )
    own_all = own_all.reshape(tp_size * row_count, model_width)
    mixer_term = jnp.dot(attended, mixer_weight, preferred_element_type=jnp.float32).astype(
        jnp.bfloat16
    )
    rows = arrived.reshape(tp_size * slot_total, model_width)
    tile = slot_total
    while tile > 384 and tile % 32 == 0:
        tile = tile // 2
    part = expert_parts(
        capacity, block_slots, tile, rows, expert_gate, expert_up, expert_down
    )
    part = part.reshape(tp_size, ep_size, block_slots, model_width)
    shared_term = shared_term_of(own_all, shared_gate, shared_up, shared_down).reshape(
        tp_size, row_count, model_width
    )
    mixer_term = mixer_term.reshape(tp_size, shard_rows // tp_size, model_width)
    back_rows, shared_sum, mixer_sum = back_exchange(
        ep_size, tp_size, part, shared_term, mixer_term
    )
    back_rows = back_rows.reshape(slot_total, model_width)
    placed = slot_index[:, :, None] == slots[None, None, :]
    mixing = jnp.sum(jnp.where(placed, route_weights[:, :, None], 0.0), axis=1)
    mixing_high = mixing.astype(jnp.bfloat16)
    mixing_low = (mixing - mixing_high.astype(jnp.float32)).astype(jnp.bfloat16)
    routed = jnp.dot(mixing_high, back_rows, preferred_element_type=jnp.float32) + jnp.dot(
        mixing_low, back_rows, preferred_element_type=jnp.float32
    )
    combined = routed + shared_sum
    expert_out = root_norm(combined, exit_gain).astype(jnp.bfloat16)
    mixer_out = root_norm(mixer_sum, mixer_gain).astype(jnp.bfloat16)
    return (mixer_out, expert_out)


def solution(mesh):
    in_specs = (
        P("ep", "tp"),
        P("ep", "tp"),
        P("ep", "tp"),
        P("ep", "tp"),
        P("tp", None),
        P(),
        P(("ep", "tp"), None),
        P(),
        P(("ep", "tp"), None),
        P(("ep", "tp"), None),
        P("ep", None, "tp"),
        P("ep", None, "tp"),
        P("ep", "tp", None),
        P(None, "tp"),
        P(None, "tp"),
        P("tp", None),
        P(),
    )
    out_specs = (P(("ep", "tp"), None), P(("ep", "tp"), None))
    return jax.shard_map(
        on_device, mesh=mesh, in_specs=in_specs, out_specs=out_specs, check_vma=False
    )
```
